512 devices in a mesh: sp: 64 (over z, y), tp: 8 (over x, core).
Axes of the slice: x: 4, y: 4, z: 16, core: 2. Of those that a mesh axis runs over, the one named last changes fastest.
Arguments:
- tokens: bfloat16 [16384, 2048], P('sp', 'tp'), may hold values from -6 to 6
- norm_gain: float32 [2, 2048], replicated, may hold values from 0.1 to 1.9
- w_bgate: bfloat16 [2, 2048, 2048], P(None, 'sp', 'tp'), may hold values from -0.125 to 0.125
- w_cgate: bfloat16 [2, 2048, 2048], P(None, 'sp', 'tp'), may hold values from -0.125 to 0.125
- w_value: bfloat16 [2, 2048, 2048], P(None, 'sp', 'tp'), may hold values from -0.125 to 0.125
- conv_taps: float32 [2, 3, 2048], replicated, may hold values from -3.5 to 3.5
- w_out: bfloat16 [2, 2048, 2048], P(None, 'sp', 'tp'), may hold values from -0.125 to 0.125
Outputs:
- mixed_out: bfloat16 [16384, 2048], P('sp', 'tp')
The draws below stay inside these ranges and needn't reach their ends.
All inputs are finite; a program needn't handle non-finite values.
Results may differ from the reference program's by a relative error of at most 0.015.
Values may be sent and summed in bfloat16 or wider, within the bound.
No kernel may reach another device: no remote copies, remote signals or barrier semaphores. Data moves between devices by JAX's collectives and lax.ppermute only.
A program may use at most 64 MiB of HBM per device.

```python
import jax
import jax.numpy as jnp
from jax import lax

D = 2048
LAYERS = 2
SEQ = 16384


def steps_of(stream_key, dims, pieces, low, largest):
    gain, own = 1.0, jax.random.fold_in(stream_key, 6)
    for axis_at, blocks in pieces:
        heights = jnp.exp(jax.random.uniform(jax.random.fold_in(own, axis_at), (blocks,), jnp.float32, low / len(pieces), largest / len(pieces)))
        gain = gain * jnp.repeat(heights, dims[axis_at] // blocks).reshape([-1 if axis == axis_at else 1 for axis in range(len(dims))])
    return gain


def bell_draw(stream_key, dims, width, limit, shards=(), kind=jnp.bfloat16):
    loudness = steps_of(stream_key, dims, shards, -0.22, 0.18) if shards else 1.0
    entries = jax.random.normal(stream_key, dims, jnp.float32) * width * loudness
    return jnp.minimum(jnp.maximum(entries, -limit), limit).astype(kind)


def setup_inputs(seed: int = 0) -> dict:
    key_of = jax.random.split(jax.random.key(seed), 8)
    tokens = bell_draw(key_of[0], (SEQ, D), 1.0, 6.0, ((0, 64), (1, 8)))
    norm_gain = jnp.clip(1.0 + 0.18 * jax.random.normal(key_of[1], (LAYERS, D), jnp.float32), 0.1, 1.9)
    w_bgate = bell_draw(key_of[2], (LAYERS, D, D), D ** -0.5, 0.125, ((1, 64), (2, 8)))
    w_cgate = bell_draw(key_of[3], (LAYERS, D, D), D ** -0.5, 0.125, ((1, 64), (2, 8)))
    w_value = bell_draw(key_of[4], (LAYERS, D, D), D ** -0.5, 0.125, ((1, 64), (2, 8)))
    conv_taps = bell_draw(key_of[5], (LAYERS, 3, D), 3 ** -0.5, 3.5, (), jnp.float32)
    w_out = bell_draw(key_of[6], (LAYERS, D, D), D ** -0.5, 0.125, ((1, 64), (2, 8)))
    return {"tokens": tokens, "norm_gain": norm_gain, "w_bgate": w_bgate, "w_cgate": w_cgate, "w_value": w_value, "conv_taps": conv_taps, "w_out": w_out}


def reference(tokens, norm_gain, w_bgate, w_cgate, w_value, conv_taps, w_out):
    current = tokens
    for layer_idx in range(LAYERS):
        as_float = current.astype(jnp.float32)
        scale = lax.rsqrt(lax.optimization_barrier(jnp.mean(as_float * as_float, axis=-1, keepdims=True)) + 1e-06)
        normed = (as_float * scale * norm_gain[layer_idx].astype(jnp.float32)).astype(jnp.bfloat16)
        bgate = lax.optimization_barrier(jnp.dot(normed, w_bgate[layer_idx], preferred_element_type=jnp.float32).astype(jnp.bfloat16))
        cgate = lax.optimization_barrier(jnp.dot(normed, w_cgate[layer_idx], preferred_element_type=jnp.float32).astype(jnp.bfloat16))
        values = lax.optimization_barrier(jnp.dot(normed, w_value[layer_idx], preferred_element_type=jnp.float32).astype(jnp.bfloat16))
        product = cgate.astype(jnp.float32) * values.astype(jnp.float32)
        padded = jnp.pad(product, ((2, 0), (0, 0)))
        taps = conv_taps[layer_idx]
        mixed = taps[0] * padded[:-2] + taps[1] * padded[1:-1] + taps[2] * padded[2:]
        gated = (bgate.astype(jnp.float32) * mixed).astype(jnp.bfloat16)
        update = jnp.dot(gated, w_out[layer_idx], preferred_element_type=jnp.float32)
        current = (as_float + update).astype(jnp.bfloat16)
    return current
```

```python
import functools

import jax
import jax.numpy as jnp
from jax import lax
from jax.experimental import pallas as pl
from jax.experimental.pallas import tpu as pltpu
from jax.sharding import Mesh
from jax.sharding import PartitionSpec as P


NZ, NY, NX = 16, 4, 4
FAR = (0, 4, 8, 12)
NEAR = (0, 1, 2, 15)
FRINGE = 16
BF, F32 = jnp.bfloat16, jnp.float32


def from_z(shard, distance):
    if distance == 0:
        return shard
    return lax.ppermute(shard, "z", [(i, (i + distance) % NZ) for i in range(NZ)])


def from_other_core(shard):
    return lax.ppermute(shard, "c", [(0, 1), (1, 0)])


def copies_of_all(shard, axis, size):
    copies = jnp.broadcast_to(shard, (size, *shard.shape))
    return lax.all_to_all(copies, axis, split_axis=0, concat_axis=0, tiled=True)


def weights_of_layer(first, second):
    both = jnp.stack([first, second])
    far = [from_z(both, d) for d in FAR]
    far_first = jnp.stack([f[0] for f in far])
    far_second = jnp.stack([f[1] for f in far])
    second_all = copies_of_all(far_second, "y", NY)
    near_first = jnp.stack([from_z(far_first, d) for d in NEAR])
    second_near = [from_z(second_all, d) for d in NEAR]
    first_all = copies_of_all(near_first, "y", NY)
    return first_all, second_near


def gathered(shard):
    own = copies_of_all(shard, "x", NX)
    return own, from_other_core(own)


def z_of(my_z, near, far):
    return lax.rem(my_z + (2 * NZ - NEAR[near] - FAR[far]), NZ)


def lanes(block, width):
    return pl.ds(pl.multiple_of(block * width, width), width)


def lhs_pair(all_ref, my_z, near, pair):
    return jnp.concatenate(
        [all_ref[:, lanes(z_of(my_z, near, 2 * pair + i), 128)] for i in range(2)], axis=1
    )


def rows_of(ref, index):
    return jnp.concatenate([ref[index(y, far)] for far in range(2) for y in range(NY)], axis=0)


def gates_kernel(layer, place, own, oth, gain, taps, first, s0, s1, s2, s3, out, normed):
    my_z, my_x, my_c = place[0], place[1], place[2]
    rows = own.shape[1]
    total = jnp.zeros((rows, 256), F32)
    for ref in (own, oth):
        for x in range(NX):
            v = ref[x].astype(F32)
            total = total + v * v
    scale = lax.rsqrt(jnp.sum(total, axis=-1, keepdims=True) * (1.0 / 2048.0) + 1e-06)
    for ref, core in ((own, my_c), (oth, 1 - my_c)):
        for x in range(NX):
            at = lanes(2 * x + core, 256)
            normed[:, at] = (ref[x].astype(F32) * scale * gain[layer : layer + 1, at]).astype(BF)
    sums = [jnp.zeros((rows, 256), F32) for _ in range(3)]
    seconds = (s0, s1, s2, s3)
    for near in range(4):
        for pair in range(2):
            lhs = lhs_pair(normed, my_z, near, pair)
            rights = (
                rows_of(first, lambda y, f: (y, near, 2 * pair + f, 0)),
                rows_of(first, lambda y, f: (y, near, 2 * pair + f, 1)),
                rows_of(seconds[near], lambda y, f: (y, 2 * pair + f, 0)),
            )
            for i in range(3):
                sums[i] = sums[i] + jnp.dot(lhs, rights[i], preferred_element_type=F32)
    cgate, values, bgate = (s.astype(BF).astype(F32) for s in sums)
    product = cgate * values
    at = lanes(2 * my_x + my_c, 256)
    taps = [taps[layer, k : k + 1, at] for k in range(3)]
    zero = jnp.zeros((8, 256), F32)
    padded = jnp.concatenate([zero, product], axis=0)
    mixed = taps[0] * padded[6 : 6 + rows] + taps[1] * padded[7 : 7 + rows] + taps[2] * product
    out[...] = (bgate * mixed).astype(BF)


def out_kernel(skip, place, own, oth, current, s0, s1, s2, s3, out, whole):
    my_z, my_c = place[0], place[2]
    rows = own.shape[1]
    for ref, core in ((own, my_c), (oth, 1 - my_c)):
        for x in range(NX):
            whole[:, lanes(2 * x + core, 256)] = ref[x]
    total = jnp.zeros((rows, 256), F32)
    seconds = (s0, s1, s2, s3)
    for near in range(4):
        for pair in range(2):
            lhs = lhs_pair(whole, my_z, near, pair)
            right = rows_of(seconds[near], lambda y, f: (y, 2 * pair + f, 1))
            total = total + jnp.dot(lhs, right, preferred_element_type=F32)
    out[...] = (current[...].astype(F32) + total).astype(BF)[skip:]


def call(body, shape, scratch, name, *args):
    vmem = pl.BlockSpec(memory_space=pltpu.VMEM)
    smem = pl.BlockSpec(memory_space=pltpu.SMEM)
    return pl.pallas_call(
        body,
        out_shape=jax.ShapeDtypeStruct(shape, BF),
        in_specs=[smem] + [vmem] * (len(args) - 1),
        out_specs=vmem,
        scratch_shapes=[pltpu.VMEM(scratch, BF)],
        compiler_params=pltpu.CompilerParams(vmem_limit_bytes=40 << 20),
        name=name,
    )(*args)


def shards(tokens, norm_gain, w_bgate, w_cgate, w_value, conv_taps, w_out):
    depth = w_bgate.shape[0]
    place = jnp.stack([lax.axis_index("z"), lax.axis_index("x"), lax.axis_index("c")]).astype(jnp.int32)
    fringe = lax.ppermute(
        tokens[-FRINGE:], ("z", "y"), [(i, i + 1) for i in range(NZ * NY - 1)]
    )
    current = jnp.concatenate([fringe, tokens], axis=0)
    rows = current.shape[0]
    weights = [
        weights_of_layer(
            jnp.stack([w_cgate[n], w_value[n]]), jnp.stack([w_bgate[n], w_out[n]])
        )
        for n in range(depth)
    ]
    for n in range(depth):
        first, second = weights[n]
        own, oth = gathered(current)
        gated = call(
            functools.partial(gates_kernel, n), (rows, 256), (rows, 2048), "gates",
            place, own, oth, norm_gain, conv_taps, first, *second,
        )
        own, oth = gathered(gated)
        skip = FRINGE if n == depth - 1 else 0
        current = call(
            functools.partial(out_kernel, skip), (rows - skip, 256), (rows, 2048), "out",
            place, own, oth, current, *second,
        )
    return current


def solution(mesh):
    grid = Mesh(mesh.devices.reshape(NZ, NY, NX, 2), ("z", "y", "x", "c"))
    weight = P(None, ("z", "y"), ("x", "c"))
    tokens = P(("z", "y"), ("x", "c"))
    return jax.shard_map(
        shards,
        mesh=grid,
        in_specs=(tokens, P(), weight, weight, weight, P(), weight),
        out_specs=tokens,
        check_vma=False,
    )
```
